32 devices in a mesh: grp: 2 (over x), ep: 8 (over z, y), tp: 2 (over core).
Axes of the slice: x: 2, y: 2, z: 4, core: 2. Of those that a mesh axis runs over, the one named last changes fastest.
Arguments:
- tokens: bfloat16 [8192, 2048], P(('grp', 'ep', 'tp')), parts along dimension 0, may hold values from -6 to 6
- norm_gain: float32 [2048], replicated, may hold values from 0.1 to 1.9
- expert_ids: int32 [8192, 4], P(('grp', 'ep', 'tp')), parts along dimension 0, may hold values from 0 to 31, all different within a row; in each aligned block of 256 rows (0 to 255, 256 to 511, ...) at most 40 rows name the same one
- gate_weights: float32 [8192, 4], P(('grp', 'ep', 'tp')), parts along dimension 0, may hold values from 0.1 to 1
- expert_gate: bfloat16 [32, 2048, 512], P('ep', None, 'tp'), may hold values from -0.125 to 0.125
- expert_up: bfloat16 [32, 2048, 512], P('ep', None, 'tp'), may hold values from -0.125 to 0.125
- expert_down: bfloat16 [32, 512, 2048], P('ep', 'tp'), may hold values from -0.25 to 0.25
- shared_gate: bfloat16 [2048, 512], replicated, may hold values from -0.125 to 0.125
- shared_up: bfloat16 [2048, 512], replicated, may hold values from -0.125 to 0.125
- shared_down: bfloat16 [512, 2048], replicated, may hold values from -0.25 to 0.25
- post_gain: float32 [2048], replicated, may hold values from 0.1 to 1.9
Outputs:
- mixed: bfloat16 [8192, 2048], P(('grp', 'ep', 'tp')), parts along dimension 0
The draws below stay inside these ranges and needn't reach their ends.
There are 2 independent parts, one for each index of `grp`. The reference program is written for one: setup_inputs(seed, part) draws one part's arguments, and reference() takes and returns one part's arrays. A program takes and returns all parts, laid end to end along the dimension named above; an argument that names none is the same for every part. Nothing has to cross between parts.
Inputs may be any that keep to these rules, and one draw needn't show every extreme that they name: `expert_ids`: each row names 4 different experts; in each device's aligned block of 256 rows no expert is named by more than 40 rows, a bound that some block reaches.
All inputs are finite; a program needn't handle non-finite values.
Results may differ from the reference program's by a relative error of at most 0.0067.
Values may be sent and summed in bfloat16 or wider, within the bound.
A program may use at most 128 MiB of HBM per device.

```python
import math
import jax
import jax.numpy as jnp
import numpy as np
from jax import lax

D = 2048
FE = 512
FS = 512
EXPERTS = 32
TOP_K = 4
TOK_DEV = 256
CAP = 40
TOKENS = 4096


def shard_levels(stream_key, dims, split, low, top_value):
    def one(axis_at, blocks):
        heights = jax.random.uniform(jax.random.fold_in(jax.random.fold_in(stream_key, 6), axis_at), (blocks,), jnp.float32, low / len(split), top_value / len(split))
        return jnp.repeat(jnp.exp(heights), dims[axis_at] // blocks).reshape((-1,) + (1,) * (len(dims) - axis_at - 1))

    level = one(*split[0])
    for cut in split[1:]:
        level = level * one(*cut)
    return level


def assign_block(rng, own, number, rows, amount, top, limit, lean):
    sequence = jax.random.permutation(rng, amount)
    heavy_load, common = load_shares(amount, rows * top, limit, lean, True), load_shares(amount, rows * top, limit, lean, False)
    places = jnp.arange(amount)

    def named(sizes, offset_by):
        used = int((sizes > 0).sum())
        fixed = max(1, used // 4)
        moved = fixed + (places - fixed + offset_by * (used - fixed)) % max(1, amount - fixed)
        return jnp.zeros((amount,), jnp.int32).at[sequence[jnp.where(places < fixed, places, moved)]].set(jnp.asarray(sizes, jnp.int32))

    sizes = jnp.where(number % 4 == 0, named(heavy_load, number // 4), named(common, number - number // 4 - 1))
    mixed = jax.random.permutation(jax.random.fold_in(own, 3), amount)
    source_of, taker = mixed[0:amount // 2 * 2:2], mixed[1:amount // 2 * 2:2]
    margin = jnp.minimum(sizes[source_of] - 1, limit - sizes[taker]) // 2
    margin = jnp.where((source_of == sequence[0]) | (taker == sequence[0]) | (sizes[taker] == 0), 0, jnp.maximum(margin, 0))
    moved = jax.random.randint(jax.random.fold_in(own, 4), (amount // 2,), 0, 1 << 20) % (margin + 1)
    sizes = sizes.at[source_of].add(-moved).at[taker].add(moved)
    items = jnp.searchsorted(jnp.cumsum(sizes), jnp.arange(rows * top), side="right").astype(jnp.int32)
    table = items.reshape(top, rows).T
    table = table[jax.random.permutation(jax.random.fold_in(own, 1), rows)]
    offset_by = jax.random.randint(jax.random.fold_in(own, 2), (rows, 1), 0, top)
    return jnp.take_along_axis(table, (jnp.arange(top)[None, :] + offset_by) % top, axis=1)


def load_shares(number_of, total, bound, skew, full):
    weights = [(1 << 20) // math.isqrt(rank ** skew) + 1 for rank in range(1, number_of + 1)]
    largest = bound if full else min(bound, max(-(-total // number_of), total * weights[0] // sum(weights)))
    least = 1 if total - largest >= number_of - 1 else 0
    holding, rest = [largest] + [least] * (number_of - 1), total - largest - least * (number_of - 1)
    while rest > 0:
        free = [i for i in range(1, number_of) if holding[i] < largest] or [i for i in range(1, number_of) if holding[i] < bound]
        pool, left = sum([weights[i] for i in free]), rest
        for i in free:
            more = min(bound - holding[i], max(1, left * weights[i] // pool), rest)
            holding[i] = holding[i] + more
            rest = rest - more
    return np.array(holding)


def gaussian(own_key, dims, scale, reach, shards=(), kind=jnp.bfloat16):
    drawn = jax.random.normal(own_key, dims, jnp.float32) * scale
    if len(shards) > 0:
        drawn = shard_levels(own_key, dims, shards, -0.22, 0.18) * drawn
    return jnp.clip(drawn, min=-reach, max=reach).astype(kind)


def setup_inputs(seed: int = 0, part: int = 0) -> dict:
    streams_of = jax.random.split(jax.random.key(seed), 12)
    own_keys = jax.random.split(jax.random.fold_in(streams_of[11], part), 12)
    tokens = gaussian(own_keys[0], (TOKENS, D), 1.0, 6.0, ((0, 16),))
    norm_gain = jnp.clip(1.0 + 0.18 * jax.random.normal(streams_of[1], (D,), jnp.float32), 0.1, 1.9)
    expert_ids_keys = jax.random.split(jax.random.fold_in(own_keys[2], 1), TOKENS // TOK_DEV)
    expert_ids_turns = jax.random.permutation(jax.random.fold_in(own_keys[2], 3), TOKENS // TOK_DEV)
    expert_ids = jax.vmap(lambda own, number: assign_block(jax.random.fold_in(own_keys[2], 2), own, number, TOK_DEV, EXPERTS, TOP_K, CAP, 1))(expert_ids_keys, expert_ids_turns).reshape((TOKENS, TOP_K))
    gate_weights = jnp.clip(jnp.exp(math.log(1.0) - 2.3025851 * jax.random.uniform(own_keys[3], (TOKENS, TOP_K), jnp.float32) ** shard_levels(own_keys[3], (TOKENS, TOP_K), ((0, 16),), -0.2, 0.2)), 0.1, 1.0)
    expert_gate = gaussian(streams_of[4], (EXPERTS, D, FE), D ** -0.5, 0.125, ((0, 8), (2, 2)))
    expert_up = gaussian(streams_of[5], (EXPERTS, D, FE), D ** -0.5, 0.125, ((0, 8), (2, 2)))
    expert_down = gaussian(streams_of[6], (EXPERTS, FE, D), FE ** -0.5, 0.25, ((0, 8), (1, 2)))
    shared_gate = gaussian(streams_of[7], (D, FS), D ** -0.5, 0.125)
    shared_up = gaussian(streams_of[8], (D, FS), D ** -0.5, 0.125)
    shared_down = gaussian(streams_of[9], (FS, D), FS ** -0.5, 0.25)
    post_gain = jnp.clip(1.0 + 0.18 * jax.random.normal(streams_of[10], (D,), jnp.float32), 0.1, 1.9)
    return dict(tokens=tokens, norm_gain=norm_gain, expert_ids=expert_ids, gate_weights=gate_weights, expert_gate=expert_gate, expert_up=expert_up, expert_down=expert_down, shared_gate=shared_gate, shared_up=shared_up, shared_down=shared_down, post_gain=post_gain)


EPS = 1e-06

def rms_scale(inputs, gain):
    mean_sq = lax.optimization_barrier(jnp.mean(inputs * inputs, axis=-1, keepdims=True))
    return inputs * lax.rsqrt(mean_sq + EPS) * gain.astype(jnp.float32)

def swiglu_out(tok_rows, w_gate, w_up, w_down):
    gate_act = jnp.dot(tok_rows, w_gate, preferred_element_type=jnp.float32)
    up_act = jnp.dot(tok_rows, w_up, preferred_element_type=jnp.float32)
    hidden = (jax.nn.silu(gate_act) * up_act).astype(jnp.bfloat16)
    return jnp.dot(hidden, w_down, preferred_element_type=jnp.float32)

def reference(tokens, norm_gain, expert_ids, gate_weights, expert_gate, expert_up, expert_down, shared_gate, shared_up, shared_down, post_gain):
    tok_total = tokens.shape[0]
    width = tokens.shape[1]
    blocks = tok_total // TOK_DEV
    normed = rms_scale(tokens.astype(jnp.float32), norm_gain).astype(jnp.bfloat16)
    ids_blocked = expert_ids.reshape(blocks, TOK_DEV * TOP_K)
    onehot = (ids_blocked[:, :, None] == jnp.arange(EXPERTS, dtype=jnp.int32)[None, None, :]).astype(jnp.int32)
    slot_index = lax.optimization_barrier(jnp.sum(jnp.cumsum(onehot, axis=1) * onehot, axis=2)) - 1
    block_index = jnp.arange(blocks, dtype=jnp.int32)[:, None]
    position = (ids_blocked * (blocks * CAP) + block_index * CAP + slot_index).reshape(-1)
    source_row = (block_index * TOK_DEV + jnp.arange(TOK_DEV * TOP_K, dtype=jnp.int32)[None, :] // TOP_K).reshape(-1)
    lookup = jnp.full((EXPERTS * blocks * CAP,), tok_total, jnp.int32).at[position].set(source_row)
    lookup = lookup.reshape(EXPERTS, blocks * CAP)
    weight_table = jnp.zeros((EXPERTS * blocks * CAP,), jnp.float32).at[position].set(gate_weights.reshape(-1))
    weight_table = weight_table.reshape(EXPERTS, blocks * CAP)
    padded = jnp.concatenate([normed, jnp.zeros((1, width), jnp.bfloat16)], axis=0)

    def add_expert(combined, inputs):
        table_rows, table_weights, w_gate, w_up, w_down = inputs
        result = swiglu_out(padded[table_rows], w_gate, w_up, w_down).astype(jnp.bfloat16)
        combined = combined.at[table_rows].add(table_weights[:, None] * result.astype(jnp.float32))
        return (combined, None)
    start = jnp.zeros((tok_total + 1, width), jnp.float32)
    combined, _ = lax.scan(add_expert, start, (lookup, weight_table, expert_gate, expert_up, expert_down))
    shared_out = swiglu_out(normed, shared_gate, shared_up, shared_down)
    combined = combined[:tok_total] + shared_out
    return rms_scale(combined, post_gain).astype(jnp.bfloat16)
```

```python
import functools

import jax
import jax.numpy as jnp
from jax import lax
from jax.experimental import pallas as pl
from jax.experimental.pallas import tpu as pltpu
from jax.sharding import PartitionSpec as P

EXPERTS = 32
CAP = 40


EPS = 1e-06


def rms_scale(inputs, gain):
    mean_sq = jnp.mean(inputs * inputs, axis=-1, keepdims=True)
    return inputs * lax.rsqrt(mean_sq + EPS) * gain


def expert_rows(tok_rows, w_gate, w_up, w_down):
    gate_act = jnp.einsum("erd,edf->erf", tok_rows, w_gate, preferred_element_type=jnp.float32)
    up_act = jnp.einsum("erd,edf->erf", tok_rows, w_up, preferred_element_type=jnp.float32)
    hidden = (jax.nn.silu(gate_act) * up_act).astype(jnp.bfloat16)
    return jnp.einsum("erf,efd->erd", hidden, w_down, preferred_element_type=jnp.float32)


def shared_branch(normed, shared_gate, shared_up, shared_down):
    shared_act = jnp.dot(normed, shared_gate, preferred_element_type=jnp.float32)
    shared_lift = jnp.dot(normed, shared_up, preferred_element_type=jnp.float32)
    shared_hidden = (jax.nn.silu(shared_act) * shared_lift).astype(jnp.bfloat16)
    return jnp.dot(shared_hidden, shared_down, preferred_element_type=jnp.float32)


def body(
    tokens,
    norm_gain,
    expert_ids,
    gate_weights,
    expert_gate,
    expert_up,
    expert_down,
    shared_gate,
    shared_up,
    shared_down,
    post_gain,
):
    tok_count = tokens.shape[0]
    top_count = expert_ids.shape[1]
    width = tokens.shape[1]
    normed = rms_scale(tokens.astype(jnp.float32), norm_gain).astype(jnp.bfloat16)
    flat_ids = expert_ids.reshape(-1)
    onehot = (flat_ids[:, None] == jnp.arange(EXPERTS, dtype=jnp.int32)[None, :]).astype(jnp.int32)
    slot_index = jnp.sum(jnp.cumsum(onehot, axis=0) * onehot, axis=1) - 1
    position = flat_ids * CAP + slot_index
    source_row = jnp.arange(tok_count * top_count, dtype=jnp.int32) // top_count
    lookup = jnp.full((EXPERTS * CAP,), tok_count, jnp.int32).at[position].set(source_row)
    padded = jnp.concatenate([normed, jnp.zeros((1, width), jnp.bfloat16)], axis=0)
    outgoing = padded[lookup].reshape(EXPERTS, 1, CAP, width)
    whole_gate, whole_up, whole_down = (
        lax.all_gather(expert_gate, "tp", axis=2, tiled=True),
        lax.all_gather(expert_up, "tp", axis=2, tiled=True),
        lax.all_gather(expert_down, "tp", axis=1, tiled=True),
    )
    arrived = lax.all_to_all(outgoing, "ep", split_axis=0, concat_axis=1, tiled=True)
    local_experts = arrived.shape[0]
    senders = arrived.shape[1]
    slots = arrived.shape[2]
    tok_rows = arrived.reshape(local_experts, senders * slots, width)
    result = expert_rows(tok_rows, whole_gate, whole_up, whole_down).astype(jnp.bfloat16)
    result = result.reshape(local_experts, senders, slots, width)
    returned = lax.all_to_all(result, "ep", split_axis=1, concat_axis=0, tiled=True)
    shared_out = shared_branch(normed, shared_gate, shared_up, shared_down)
    back_rows = returned.reshape(EXPERTS * CAP, width)
    picked = back_rows[position].reshape(tok_count, top_count, width).astype(jnp.float32)
    routed = jnp.einsum("tk,tkd->td", gate_weights, picked)
    combined = routed + shared_out
    return rms_scale(combined, post_gain).astype(jnp.bfloat16)

VMEM_ALL = 67043328
MESH = pl.DeviceIdType.MESH


def ring_bytes(shapes):
    total = 0
    for shape, kind in shapes:
        count = jnp.dtype(kind).itemsize
        for size in shape:
            count *= size
        total += count
    return total


ROLES = ("tokens", "shared", "expert", "give", "total", "finish", "weights", "own")
TOKENS_AT, SHARED_AT, EXPERT_AT, GIVE_AT, TOTAL_AT, FINISH_AT, WEIGHTS_AT, OWN_AT = range(8)


def plain_order(nz, chunks, z):
    near = sorted(range(nz), key=lambda s: (abs(s - z), s))
    far = sorted((s for s in range(nz) if s != z), key=lambda s: (-abs(s - z), s)) + [z]
    steps = [(OWN_AT, z, c) for c in range(chunks)] if 0 < z < nz - 1 else []
    steps += [(TOKENS_AT, z, c) for c in range(chunks)] + [(SHARED_AT, z, 0)]
    steps += [(TOKENS_AT, s, c) for s in near[1:2] for c in range(chunks)] + [(WEIGHTS_AT, z, 0)]
    for k, s in enumerate(near):
        steps += [(EXPERT_AT, s, c) for c in range(chunks)]
        if s != z:
            steps += [(GIVE_AT, s, c) for c in range(chunks)]
        steps += [(TOKENS_AT, q, c) for q in near[k + 2 : k + 3] for c in range(chunks)]
    steps += [(GIVE_AT, z, c) for c in range(chunks)]
    steps += [(TOTAL_AT, s, c) for s in far for c in range(chunks)]
    return steps + [(FINISH_AT, z, 0)]


def step_tables(nz, chunks, z):
    orders = [ORDERS(nz, chunks, q) for q in range(nz)]
    length = max(len(order) for order in orders)
    size = len(ROLES) * nz * chunks + 1
    per = 1
    while size ** (per + 1) < 1 << 31:
        per += 1
    count = -(-length // per)
    packed = []
    for order in orders:
        flat = [(role * nz + s) * chunks + c for role, s, c in order]
        flat += [size - 1] * (count * per - len(flat))
        packed.append([sum(v * size**i for i, v in enumerate(flat[k * per : (k + 1) * per])) for k in range(count)])

    def step_of(k):
        group, inside = k // per, k % per
        row = []
        for i in range(count):
            value = jnp.int32(packed[0][i])
            for q in range(1, nz):
                value = jnp.where(z == q, packed[q][i], value)
            row.append(value)
        bit = 1
        while len(row) > 1:
            odd = group // bit % 2 == 1
            row = [jnp.where(odd, row[i + 1], row[i]) if i + 1 < len(row) else row[i] for i in range(0, len(row), 2)]
            bit *= 2
        code = row[0]
        for i in range(per - 1):
            code = jnp.where(inside > i, code // size, code)
        code = code % size
        return code // (nz * chunks), code // chunks % nz, code % chunks

    return length, step_of


def grid_kernel(
    nz,
    top,
    chunks,
    tok_ref,
    ids_ref,
    weights_ref,
    ngain_ref,
    pgain_ref,
    eg_hbm,
    eu_hbm,
    ed_hbm,
    sg_hbm,
    su_hbm,
    sd_hbm,
    out_ref,
    wg,
    wu,
    wd,
    sg,
    su,
    sd,
    blk,
    xa,
    xb,
    xcat,
    gate_sum,
    up_sum,
    yout,
    back,
    mine,
    pick_own,
    pick_par,
    put_own,
    put_par,
    scale,
    meta_a,
    meta_b,
    rs_in,
    shared,
    hid,
    hidden,
    acc,
    load_sem,
    w_send,
    w_recv,
    ag_send,
    ag_recv,
    mt_send,
    mt_recv,
    mb_send,
    mb_recv,
    d_send,
    d_recv,
    r_send,
    r_recv,
    rs_send,
    rs_recv,
):
    rows, width = tok_ref.shape
    experts = eg_hbm.shape[0]
    fh = eg_hbm.shape[2]
    fs = sg.shape[1]
    cw = width // chunks
    slots = experts * CAP
    step_rows = 32
    ep = lax.axis_index("ep")
    tp = lax.axis_index("tp")
    z, y = ep // 2, ep % 2
    par = ep + 1 - 2 * y
    above, below = z < nz - 1, z > 0
    up, dn = jnp.minimum(ep + 2, 2 * nz - 1), jnp.maximum(ep - 2, 0)
    partner = 1 - tp

    barrier = pltpu.get_barrier_semaphore()
    pl.semaphore_signal(barrier, inc=1, device_id={"ep": par}, device_id_type=MESH)
    pl.semaphore_signal(barrier, inc=1, device_id={"tp": partner}, device_id_type=MESH)

    @pl.when(above)
    def _():
        pl.semaphore_signal(barrier, inc=1, device_id={"ep": up}, device_id_type=MESH)

    @pl.when(below)
    def _():
        pl.semaphore_signal(barrier, inc=1, device_id={"ep": dn}, device_id_type=MESH)

    loads = [
        pltpu.make_async_copy(src, dst, load_sem.at[k])
        for k, (src, dst) in enumerate(
            (
                (sg_hbm, sg),
                (su_hbm, su),
                (sd_hbm, sd),
                (eg_hbm, wg.at[0]),
                (eu_hbm, wu.at[0]),
                (ed_hbm, wd.at[0]),
            )
        )
    ]
    for load in loads:
        load.start()

    @pl.loop(0, rows // step_rows)
    def _(r):
        at = pl.ds(pl.multiple_of(r * step_rows, step_rows), step_rows)
        v = rms_scale(tok_ref[at, :].astype(jnp.float32), ngain_ref[...]).astype(jnp.bfloat16)
        for c in range(chunks):
            blk[z, c, at, :] = v[:, c * cw : (c + 1) * cw]

    def remote(src, dst, send, recv, ep_to):
        return pltpu.make_async_remote_copy(
            src_ref=src,
            dst_ref=dst,
            send_sem=send,
            recv_sem=recv,
            device_id={"ep": ep_to},
            device_id_type=MESH,
        )

    def token_copy(way, s, c):
        return remote(blk.at[s, c], blk.at[s, c], ag_send.at[way, s, c], ag_recv.at[s, c], (up, dn)[way])

    def meta_copy(way, s):
        return remote(meta_a.at[s], meta_a.at[s], mt_send.at[way, s], mt_recv.at[s], (up, dn)[way])

    def meta_across(s):
        return remote(meta_a.at[s], meta_b.at[s], mb_send.at[s], mb_recv.at[s], par)

    def give_rows(s, c):
        return remote(yout.at[s, c], xb.at[s, c], d_send.at[s, c], d_recv.at[s, c], par)

    def give_back(s, c):
        return remote(yout.at[s, c], back.at[s, c], r_send.at[s, c], r_recv.at[s, c], par)

    def sum_copy(way, s, c, slot):
        return remote(blk.at[s, c], rs_in.at[slot, c], rs_send.at[s, c], rs_recv.at[slot, c], (up, dn)[way])

    pl.semaphore_wait(barrier, 2 + above.astype(jnp.int32) + below.astype(jnp.int32))

    low = 2 * z < nz
    for way, there, early in ((0, above, low), (1, below, ~low)):

        @pl.when(there & (early | ~above | ~below))
        def _():
            token_copy(way, z, 0).start()

    total_experts = 2 * nz * experts
    ids, weights = ids_ref[...].astype(jnp.float32), weights_ref[...]
    names = lax.broadcasted_iota(jnp.int32, (total_experts, rows), 0).astype(jnp.float32)
    named = jnp.zeros((total_experts, rows), jnp.float32)
    for k in range(top):
        named = jnp.where(ids[k : k + 1] == names, 1.0, named)
    before = lax.broadcasted_iota(jnp.int32, (rows, rows), 0) < lax.broadcasted_iota(jnp.int32, (rows, rows), 1)
    before = jnp.where(before, 1.0, 0.0).astype(jnp.bfloat16)
    rank = jnp.dot(named.astype(jnp.bfloat16), before, preferred_element_type=jnp.float32)
    for k in range(top):
        found = jnp.sum(jnp.where(ids[k : k + 1] == names, rank, 0.0), axis=0, keepdims=True)
        meta_a[z, k : k + 1, :] = ids[k : k + 1] * CAP + found
    meta_a[z, top : 2 * top, :] = weights

    for way, there in enumerate((above, below)):

        @pl.when(there)
        def _():
            meta_copy(way, z).start()

    for way, there, early in ((0, above, low), (1, below, ~low)):

        @pl.when(there & (early | ~above | ~below))
        def _():
            @pl.loop(1, chunks)
            def _(c):
                token_copy(way, z, c).start()

    swaps = [
        pltpu.make_async_remote_copy(
            src_ref=src,
            dst_ref=dst.at[1],
            send_sem=w_send.at[k],
            recv_sem=w_recv.at[k],
            device_id={"tp": partner},
            device_id_type=MESH,
        )
        for k, (src, dst) in enumerate(((eg_hbm, wg), (eu_hbm, wu), (ed_hbm, wd)))
    ]

    for swap in swaps:
        swap.start()

    def own_tokens(c):
        @pl.when(low)
        def _():
            token_copy(1, z, c).start()

        @pl.when(~low)
        def _():
            token_copy(0, z, c).start()

    def pick_table(table, owner):
        want = lax.broadcasted_iota(jnp.int32, (slots, rows), 0).astype(jnp.float32)
        want = want + (owner * slots).astype(jnp.float32)
        hits = [table[k : k + 1] == want for k in range(top)]
        mass = jnp.zeros((slots, rows), jnp.float32)
        for k in range(top):
            mass = jnp.where(hits[k], table[top + k : top + k + 1], mass)
        pick = functools.reduce(jnp.logical_or, hits)
        return jnp.where(pick, 1.0, 0.0).astype(jnp.bfloat16), jnp.sum(mass, axis=1, keepdims=True)

    def put_table(turned, owner):
        want = lax.broadcasted_iota(jnp.int32, (rows, slots), 1).astype(jnp.float32)
        want = want + (owner * slots).astype(jnp.float32)
        pick = functools.reduce(jnp.logical_or, [turned[:, k : k + 1] == want for k in range(top)])
        return jnp.where(pick, 1.0, 0.0).astype(jnp.bfloat16)

    def spread(column):
        return jnp.broadcast_to(column, (slots, 128)).reshape(experts, CAP, 128)

    def take_meta(s):
        @pl.when(s != z)
        def _():
            meta_copy(0, s).wait_recv()

        @pl.when((s < z) & above)
        def _():
            meta_copy(0, s).start()

        @pl.when((s > z) & below)
        def _():
            meta_copy(1, s).start()

        meta_across(s).start()
        table = meta_a[s]
        pick, mass = pick_table(table, ep)
        pick_own[s] = pick
        scale[s, :, :CAP, :] = spread(mass)
        pick_par[s] = pick_table(table, par)[0]
        turned = table.T
        put_own[s] = put_table(turned, ep)
        put_par[s] = put_table(turned, par)

    def take_tokens(s, c):
        @pl.when(s != z)
        def _():
            token_copy(0, s, c).wait_recv()

        @pl.when((s < z) & above)
        def _():
            token_copy(0, s, c).start()

        @pl.when((s > z) & below)
        def _():
            token_copy(1, s, c).start()

        @pl.when(c == 0)
        def _():
            take_meta(s)

        there = jnp.dot(pick_par[s], blk[s, c], preferred_element_type=jnp.float32)
        yout[s, c] = there.astype(jnp.bfloat16)
        give_rows(s, c).start()
        here = jnp.dot(pick_own[s], blk[s, c], preferred_element_type=jnp.float32)
        xa[s, c] = here.astype(jnp.bfloat16)

    tile = min(256, fs)

    def shared_expert():
        for load in loads[:3]:
            load.wait()

        @pl.loop(0, fs // tile)
        def _(k):
            at = pl.ds(pl.multiple_of(k * tile, tile), tile)
            x = jnp.concatenate([blk[z, c] for c in range(chunks)], axis=1)
            g = jnp.dot(x, sg[:, at], preferred_element_type=jnp.float32)
            u = jnp.dot(x, su[:, at], preferred_element_type=jnp.float32)
            hid[:, at] = (jax.nn.silu(g) * u).astype(jnp.bfloat16)

        @pl.loop(0, chunks)
        def _(c):
            at = pl.ds(pl.multiple_of(c * cw, cw), cw)
            shared[c] = jnp.dot(hid[...], sd[:, at], preferred_element_type=jnp.float32)

    def weights_here():
        for load in loads[3:]:
            load.wait()
        for swap in swaps:
            swap.wait_recv()

    gate_sum[...] = jnp.zeros_like(gate_sum)
    up_sum[...] = jnp.zeros_like(up_sum)

    def expert(s, c):
        @pl.when(c == 0)
        def _():
            meta_across(s).wait_recv()
            scale[s, :, CAP:, :] = spread(pick_table(meta_b[s], ep)[1])

        give_rows(s, c).wait_recv()
        depth = pl.ds(pl.multiple_of(c * cw, cw), cw)
        for e in range(experts):
            xcat[e, :CAP, :] = xa[s, c, e * CAP : (e + 1) * CAP, :]
            xcat[e, CAP:, :] = xb[s, c, e * CAP : (e + 1) * CAP, :]
        for e in range(experts):
            for h in range(2):
                gate_sum[h, e] += jnp.dot(xcat[e], wg[h, e, depth, :], preferred_element_type=jnp.float32)
                up_sum[h, e] += jnp.dot(xcat[e], wu[h, e, depth, :], preferred_element_type=jnp.float32)

        @pl.when(c == chunks - 1)
        def _():
            @pl.loop(0, experts)
            def _(e):
                weight = scale[s, e][:, :1]
                for h in range(2):
                    g, u = gate_sum[h, e], up_sum[h, e]
                    hidden[s, h, e] = (jax.nn.silu(g) * u * weight).astype(jnp.bfloat16)
                    gate_sum[h, e] = jnp.zeros_like(g)
                    up_sum[h, e] = jnp.zeros_like(u)

    def give(s, c):
        give_rows(s, c).wait_send()
        at = pl.ds(pl.multiple_of(c * cw, cw), cw)
        for e in range(experts):
            down = jnp.dot(hidden[s, 0, e], wd[0, e, :, at], preferred_element_type=jnp.float32)
            down += jnp.dot(hidden[s, 1, e], wd[1, e, :, at], preferred_element_type=jnp.float32)
            down = down.astype(jnp.bfloat16)
            yout[s, c, e * CAP : (e + 1) * CAP, :] = down[CAP:]
            mine[s, c, e * CAP : (e + 1) * CAP, :] = down[:CAP]
        give_back(s, c).start()

    def total(s, c):
        give_back(s, c).wait_recv()
        own = jnp.dot(put_own[s], mine[s, c], preferred_element_type=jnp.float32)
        own += jnp.dot(put_par[s], back[s, c], preferred_element_type=jnp.float32)
        acc[...] = own

        @pl.when((s >= z) & below)
        def _():
            sum_copy(0, s, c, s).wait_recv()
            acc[...] += rs_in[s, c].astype(jnp.float32)

        @pl.when((s <= z) & above)
        def _():
            slot = jnp.where(s == z, nz, s)
            sum_copy(1, s, c, slot).wait_recv()
            acc[...] += rs_in[slot, c].astype(jnp.float32)

        @pl.when((s < z) & above)
        def _():
            token_copy(0, s, c).wait_send()

        @pl.when((s > z) & below)
        def _():
            token_copy(1, s, c).wait_send()

        @pl.when(s == z)
        def _():
            shared[c] += acc[...]

        @pl.when(s != z)
        def _():
            blk[s, c] = acc[...].astype(jnp.bfloat16)

        @pl.when(s > z)
        def _():
            sum_copy(0, s, c, s).start()

        @pl.when(s < z)
        def _():
            sum_copy(1, s, c, jnp.where(s == z - 1, nz, s)).start()

    def finish():
        @pl.loop(0, rows // step_rows)
        def _(r):
            at = pl.ds(pl.multiple_of(r * step_rows, step_rows), step_rows)
            both = jnp.concatenate([shared[c, at, :] for c in range(chunks)], axis=1)
            out_ref[at, :] = rms_scale(both, pgain_ref[...]).astype(jnp.bfloat16)

    length, step_of = step_tables(nz, chunks, z)

    @pl.loop(0, length)
    def _(k):
        role, s, c = step_of(k)
        pl.when(role == TOKENS_AT)(lambda: take_tokens(s, c))
        pl.when(role == SHARED_AT)(shared_expert)
        pl.when(role == EXPERT_AT)(lambda: expert(s, c))
        pl.when(role == GIVE_AT)(lambda: give(s, c))
        pl.when(role == TOTAL_AT)(lambda: total(s, c))
        pl.when(role == FINISH_AT)(finish)
        pl.when(role == WEIGHTS_AT)(weights_here)
        pl.when(role == OWN_AT)(lambda: own_tokens(c))

    for swap in swaps:
        swap.wait_send()
    for way, there in enumerate((above, below)):

        @pl.when(there)
        def _():
            meta_copy(way, z).wait_send()

            @pl.loop(0, chunks)
            def _(c):
                token_copy(way, z, c).wait_send()

    @pl.loop(0, nz)
    def _(s):
        @pl.when((s < z) & above)
        def _():
            meta_copy(0, s).wait_send()

        @pl.when((s > z) & below)
        def _():
            meta_copy(1, s).wait_send()

        meta_across(s).wait_send()

        @pl.loop(0, chunks)
        def _(c):
            give_back(s, c).wait_send()

            @pl.when(s != z)
            def _():
                sum_copy(0, s, c, s).wait_send()


def grid_shapes(nz, chunks, rows, width, meta_rows, eg, ed, sg, sd):
    bf, f32 = jnp.bfloat16, jnp.float32
    experts = eg.shape[0]
    fs = sg.shape[1]
    cw = width // chunks
    slots = experts * CAP
    return [
        ((2,) + eg.shape, bf),
        ((2,) + eg.shape, bf),
        ((2,) + ed.shape, bf),
        (sg.shape, bf),
        (sg.shape, bf),
        (sd.shape, bf),
        ((nz, chunks, rows, cw), bf),
        ((nz, chunks, slots, cw), bf),
        ((nz, chunks, slots, cw), bf),
        ((experts, 2 * CAP, cw), bf),
        ((2, experts, 2 * CAP, eg.shape[2]), f32),
        ((2, experts, 2 * CAP, eg.shape[2]), f32),
        ((nz, chunks, slots, cw), bf),
        ((nz, chunks, slots, cw), bf),
        ((nz, chunks, slots, cw), bf),
        ((nz, slots, rows), bf),
        ((nz, slots, rows), bf),
        ((nz, rows, slots), bf),
        ((nz, rows, slots), bf),
        ((nz, experts, 2 * CAP, 128), f32),
        ((nz, meta_rows, rows), f32),
        ((nz, meta_rows, rows), f32),
        ((nz + 1, chunks, rows, cw), bf),
        ((chunks, rows, cw), f32),
        ((rows, fs), bf),
        ((nz, 2, experts, 2 * CAP, eg.shape[2]), bf),
        ((rows, cw), f32),
    ]


def grid_body(
    n,
    tokens,
    norm_gain,
    expert_ids,
    gate_weights,
    expert_gate,
    expert_up,
    expert_down,
    shared_gate,
    shared_up,
    shared_down,
    post_gain,
):
    rows, width = tokens.shape
    top = expert_ids.shape[1]
    nz = n // 2
    chunks = CHUNKS
    meta_rows = -(-2 * top // 8) * 8
    shapes = grid_shapes(nz, chunks, rows, width, meta_rows, expert_gate, expert_down, shared_gate, shared_down)
    if ring_bytes(shapes) + 4 * rows * width > VMEM_ALL - (2 << 20):
        return body(
            tokens,
            norm_gain,
            expert_ids,
            gate_weights,
            expert_gate,
            expert_up,
            expert_down,
            shared_gate,
            shared_up,
            shared_down,
            post_gain,
        )
    dma = pltpu.SemaphoreType.DMA
    vmem = pl.BlockSpec(memory_space=pltpu.VMEM)
    hbm = pl.BlockSpec(memory_space=pl.ANY)
    return pl.pallas_call(
        functools.partial(grid_kernel, nz, top, chunks),
        out_shape=jax.ShapeDtypeStruct((rows, width), jnp.bfloat16),
        in_specs=[vmem] * 5 + [hbm] * 6,
        out_specs=vmem,
        scratch_shapes=[pltpu.VMEM(shape, kind) for shape, kind in shapes]
        + [
            dma((6,)),
            dma((3,)),
            dma((3,)),
            dma((2, nz, chunks)),
            dma((nz, chunks)),
            dma((2, nz)),
            dma((nz,)),
            dma((nz,)),
            dma((nz,)),
            dma((nz, chunks)),
            dma((nz, chunks)),
            dma((nz, chunks)),
            dma((nz, chunks)),
            dma((nz, chunks)),
            dma((nz + 1, chunks)),
        ],
        compiler_params=pltpu.CompilerParams(
            collective_id=0, has_side_effects=True, vmem_limit_bytes=VMEM_ALL
        ),
    )(
        tokens,
        expert_ids.T,
        gate_weights.T,
        norm_gain.reshape(1, width),
        post_gain.reshape(1, width),
        expert_gate,
        expert_up,
        expert_down,
        shared_gate,
        shared_up,
        shared_down,
    )


CHUNKS = 4
STEPS = (
    (
        0, 3, 2, 1, 10, 100, 20, 21, 600, 22, 220, 221, 23, 222, 30, 223,
        323, 320, 321, 200, 201, 31, 423, 33, 420, 421, 32, 202, 203, 322, 12, 230,
        231, 232, 233, 333, 422, 331, 332, 11, 433, 210, 431, 13, 330, 211, 432, 212,
        213, 311, 430, 312, 310, 411, 313, 303, 412, 301, 413, 302, 410, 300, 402, 403,
        401, 400, 500,
    ),
    (
        10, 710, 12, 11, 20, 0, 21, 13, 22, 23, 110, 1, 30, 610, 3, 31,
        220, 33, 221, 2, 222, 32, 223, 200, 201, 712, 323, 320, 202, 203, 711, 321,
        230, 713, 423, 231, 232, 322, 420, 233, 210, 211, 330, 333, 332, 421, 331, 212,
        213, 422, 303, 302, 301, 311, 300, 433, 431, 312, 403, 310, 432, 313, 430, 401,
        402, 411, 412, 400, 413, 410, 510,
    ),
)


def ORDERS(nz, chunks, z):
    if nz != 2 * len(STEPS):
        return plain_order(nz, chunks, z)
    near = min(z, nz - 1 - z)
    steps = [(k // 100, k // 10 % 10, k % 10) for k in STEPS[near]]
    return [(role, s if near == z else nz - 1 - s, c) for role, s, c in steps]


def solution(mesh):
    ringed = mesh.shape["tp"] == 2 and mesh.shape["ep"] % 2 == 0 and mesh.shape["ep"] > 2
    return jax.shard_map(
        functools.partial(grid_body, mesh.shape["ep"]) if ringed else body,
        mesh=mesh,
        in_specs=(
            P(("grp", "ep", "tp"), None),
            P(),
            P(("grp", "ep", "tp"), None),
            P(("grp", "ep", "tp"), None),
            P("ep", None, "tp"),
            P("ep", None, "tp"),
            P("ep", "tp", None),
            P(),
            P(),
            P(),
            P(),
        ),
        out_specs=P(("grp", "ep", "tp"), None),
        check_vma=False,
    )
```

```python
import functools

import jax
import jax.numpy as jnp
from jax import lax
from jax.experimental import pallas as pl
from jax.experimental.pallas import tpu as pltpu
from jax.sharding import PartitionSpec as P

EXPERTS = 32
CAP = 40


EPS = 1e-06


def rms_scale(inputs, gain):
    mean_sq = jnp.mean(inputs * inputs, axis=-1, keepdims=True)
    return inputs * lax.rsqrt(mean_sq + EPS) * gain


def expert_rows(tok_rows, w_gate, w_up, w_down):
    gate_act = jnp.einsum("erd,edf->erf", tok_rows, w_gate, preferred_element_type=jnp.float32)
    up_act = jnp.einsum("erd,edf->erf", tok_rows, w_up, preferred_element_type=jnp.float32)
    hidden = (jax.nn.silu(gate_act) * up_act).astype(jnp.bfloat16)
    return jnp.einsum("erf,efd->erd", hidden, w_down, preferred_element_type=jnp.float32)


def shared_branch(normed, shared_gate, shared_up, shared_down):
    shared_act = jnp.dot(normed, shared_gate, preferred_element_type=jnp.float32)
    shared_lift = jnp.dot(normed, shared_up, preferred_element_type=jnp.float32)
    shared_hidden = (jax.nn.silu(shared_act) * shared_lift).astype(jnp.bfloat16)
    return jnp.dot(shared_hidden, shared_down, preferred_element_type=jnp.float32)


def body(
    tokens,
    norm_gain,
    expert_ids,
    gate_weights,
    expert_gate,
    expert_up,
    expert_down,
    shared_gate,
    shared_up,
    shared_down,
    post_gain,
):
    tok_count = tokens.shape[0]
    top_count = expert_ids.shape[1]
    width = tokens.shape[1]
    normed = rms_scale(tokens.astype(jnp.float32), norm_gain).astype(jnp.bfloat16)
    flat_ids = expert_ids.reshape(-1)
    onehot = (flat_ids[:, None] == jnp.arange(EXPERTS, dtype=jnp.int32)[None, :]).astype(jnp.int32)
    slot_index = jnp.sum(jnp.cumsum(onehot, axis=0) * onehot, axis=1) - 1
    position = flat_ids * CAP + slot_index
    source_row = jnp.arange(tok_count * top_count, dtype=jnp.int32) // top_count
    lookup = jnp.full((EXPERTS * CAP,), tok_count, jnp.int32).at[position].set(source_row)
    padded = jnp.concatenate([normed, jnp.zeros((1, width), jnp.bfloat16)], axis=0)
    outgoing = padded[lookup].reshape(EXPERTS, 1, CAP, width)
    whole_gate, whole_up, whole_down = (
        lax.all_gather(expert_gate, "tp", axis=2, tiled=True),
        lax.all_gather(expert_up, "tp", axis=2, tiled=True),
        lax.all_gather(expert_down, "tp", axis=1, tiled=True),
    )
    arrived = lax.all_to_all(outgoing, "ep", split_axis=0, concat_axis=1, tiled=True)
    local_experts = arrived.shape[0]
    senders = arrived.shape[1]
    slots = arrived.shape[2]
    tok_rows = arrived.reshape(local_experts, senders * slots, width)
    result = expert_rows(tok_rows, whole_gate, whole_up, whole_down).astype(jnp.bfloat16)
    result = result.reshape(local_experts, senders, slots, width)
    returned = lax.all_to_all(result, "ep", split_axis=1, concat_axis=0, tiled=True)
    shared_out = shared_branch(normed, shared_gate, shared_up, shared_down)
    back_rows = returned.reshape(EXPERTS * CAP, width)
    picked = back_rows[position].reshape(tok_count, top_count, width).astype(jnp.float32)
    routed = jnp.einsum("tk,tkd->td", gate_weights, picked)
    combined = routed + shared_out
    return rms_scale(combined, post_gain).astype(jnp.bfloat16)

VMEM_ALL = 67043328
MESH = pl.DeviceIdType.MESH


def ring_bytes(shapes):
    total = 0
    for shape, kind in shapes:
        count = jnp.dtype(kind).itemsize
        for size in shape:
            count *= size
        total += count
    return total


ROLES = ("tokens", "shared", "expert", "give", "total", "finish", "weights", "own")
TOKENS_AT, SHARED_AT, EXPERT_AT, GIVE_AT, TOTAL_AT, FINISH_AT, WEIGHTS_AT, OWN_AT = range(8)


def plain_order(nz, chunks, z):
    near = sorted(range(nz), key=lambda s: (abs(s - z), s))
    far = sorted((s for s in range(nz) if s != z), key=lambda s: (-abs(s - z), s)) + [z]
    steps = [(OWN_AT, z, c) for c in range(chunks)] if 0 < z < nz - 1 else []
    steps += [(TOKENS_AT, z, c) for c in range(chunks)] + [(SHARED_AT, z, 0)]
    steps += [(TOKENS_AT, s, c) for s in near[1:2] for c in range(chunks)] + [(WEIGHTS_AT, z, 0)]
    for k, s in enumerate(near):
        steps += [(EXPERT_AT, s, c) for c in range(chunks)]
        if s != z:
            steps += [(GIVE_AT, s, c) for c in range(chunks)]
        steps += [(TOKENS_AT, q, c) for q in near[k + 2 : k + 3] for c in range(chunks)]
    steps += [(GIVE_AT, z, c) for c in range(chunks)]
    steps += [(TOTAL_AT, s, c) for s in far for c in range(chunks)]
    return steps + [(FINISH_AT, z, 0)]


def step_tables(nz, chunks, z):
    orders = [ORDERS(nz, chunks, q) for q in range(nz)]
    length = max(len(order) for order in orders)
    size = len(ROLES) * nz * chunks + 1
    per = 1
    while size ** (per + 1) < 1 << 31:
        per += 1
    count = -(-length // per)
    packed = []
    for order in orders:
        flat = [(role * nz + s) * chunks + c for role, s, c in order]
        flat += [size - 1] * (count * per - len(flat))
        packed.append([sum(v * size**i for i, v in enumerate(flat[k * per : (k + 1) * per])) for k in range(count)])

    def step_of(k):
        group, inside = k // per, k % per
        row = []
        for i in range(count):
            value = jnp.int32(packed[0][i])
            for q in range(1, nz):
                value = jnp.where(z == q, packed[q][i], value)
            row.append(value)
        bit = 1
        while len(row) > 1:
            odd = group // bit % 2 == 1
            row = [jnp.where(odd, row[i + 1], row[i]) if i + 1 < len(row) else row[i] for i in range(0, len(row), 2)]
            bit *= 2
        code = row[0]
        for i in range(per - 1):
            code = jnp.where(inside > i, code // size, code)
        code = code % size
        return code // (nz * chunks), code // chunks % nz, code % chunks

    return length, step_of


def grid_kernel(
    nz,
    top,
    chunks,
    tok_ref,
    ids_ref,
    weights_ref,
    ngain_ref,
    pgain_ref,
    eg_hbm,
    eu_hbm,
    ed_hbm,
    sg_hbm,
    su_hbm,
    sd_hbm,
    out_ref,
    wg,
    wu,
    wd,
    sg,
    su,
    sd,
    blk,
    xa,
    xb,
    xcat,
    gate_sum,
    up_sum,
    yout,
    back,
    mine,
    pick_own,
    pick_par,
    put_own,
    put_par,
    scale,
    meta_a,
    meta_b,
    rs_in,
    shared,
    hid,
    hidden,
    acc,
    load_sem,
    w_send,
    w_recv,
    ag_send,
    ag_recv,
    mt_send,
    mt_recv,
    mb_send,
    mb_recv,
    d_send,
    d_recv,
    r_send,
    r_recv,
    rs_send,
    rs_recv,
):
    rows, width = tok_ref.shape
    experts = eg_hbm.shape[0]
    fh = eg_hbm.shape[2]
    fs = sg.shape[1]
    cw = width // chunks
    slots = experts * CAP
    step_rows = 32
    ep = lax.axis_index("ep")
    tp = lax.axis_index("tp")
    z, y = ep // 2, ep % 2
    par = ep + 1 - 2 * y
    above, below = z < nz - 1, z > 0
    up, dn = jnp.minimum(ep + 2, 2 * nz - 1), jnp.maximum(ep - 2, 0)
    partner = 1 - tp

    barrier = pltpu.get_barrier_semaphore()
    pl.semaphore_signal(barrier, inc=1, device_id={"ep": par}, device_id_type=MESH)
    pl.semaphore_signal(barrier, inc=1, device_id={"tp": partner}, device_id_type=MESH)

    @pl.when(above)
    def _():
        pl.semaphore_signal(barrier, inc=1, device_id={"ep": up}, device_id_type=MESH)

    @pl.when(below)
    def _():
        pl.semaphore_signal(barrier, inc=1, device_id={"ep": dn}, device_id_type=MESH)

    loads = [
        pltpu.make_async_copy(src, dst, load_sem.at[k])
        for k, (src, dst) in enumerate(
            (
                (sg_hbm, sg),
                (su_hbm, su),
                (sd_hbm, sd),
                (eg_hbm, wg.at[0]),
                (eu_hbm, wu.at[0]),
                (ed_hbm, wd.at[0]),
            )
        )
    ]
    for load in loads:
        load.start()

    @pl.loop(0, rows // step_rows)
    def _(r):
        at = pl.ds(pl.multiple_of(r * step_rows, step_rows), step_rows)
        v = rms_scale(tok_ref[at, :].astype(jnp.float32), ngain_ref[...]).astype(jnp.bfloat16)
        for c in range(chunks):
            blk[z, c, at, :] = v[:, c * cw : (c + 1) * cw]

    def remote(src, dst, send, recv, ep_to):
        return pltpu.make_async_remote_copy(
            src_ref=src,
            dst_ref=dst,
            send_sem=send,
            recv_sem=recv,
            device_id={"ep": ep_to},
            device_id_type=MESH,
        )

    def token_copy(way, s, c):
        return remote(blk.at[s, c], blk.at[s, c], ag_send.at[way, s, c], ag_recv.at[s, c], (up, dn)[way])

    def meta_copy(way, s):
        return remote(meta_a.at[s], meta_a.at[s], mt_send.at[way, s], mt_recv.at[s], (up, dn)[way])

    def meta_across(s):
        return remote(meta_a.at[s], meta_b.at[s], mb_send.at[s], mb_recv.at[s], par)

    def give_rows(s, c):
        return remote(yout.at[s, c], xb.at[s, c], d_send.at[s, c], d_recv.at[s, c], par)

    def give_back(s, c):
        return remote(yout.at[s, c], back.at[s, c], r_send.at[s, c], r_recv.at[s, c], par)

    def sum_copy(way, s, c, slot):
        return remote(blk.at[s, c], rs_in.at[slot, c], rs_send.at[s, c], rs_recv.at[slot, c], (up, dn)[way])

    pl.semaphore_wait(barrier, 2 + above.astype(jnp.int32) + below.astype(jnp.int32))

    swaps = [
        pltpu.make_async_remote_copy(
            src_ref=src,
            dst_ref=dst.at[1],
            send_sem=w_send.at[k],
            recv_sem=w_recv.at[k],
            device_id={"tp": partner},
            device_id_type=MESH,
        )
        for k, (src, dst) in enumerate(((eg_hbm, wg), (eu_hbm, wu), (ed_hbm, wd)))
    ]
    for swap in swaps:
        swap.start()

    low = 2 * z < nz
    for way, there, early in ((0, above, low), (1, below, ~low)):

        @pl.when(there & (early | ~above | ~below))
        def _():
            token_copy(way, z, 0).start()

    total_experts = 2 * nz * experts
    ids, weights = ids_ref[...].astype(jnp.float32), weights_ref[...]
    names = lax.broadcasted_iota(jnp.int32, (total_experts, rows), 0).astype(jnp.float32)
    named = jnp.zeros((total_experts, rows), jnp.float32)
    for k in range(top):
        named = jnp.where(ids[k : k + 1] == names, 1.0, named)
    before = lax.broadcasted_iota(jnp.int32, (rows, rows), 0) < lax.broadcasted_iota(jnp.int32, (rows, rows), 1)
    before = jnp.where(before, 1.0, 0.0).astype(jnp.bfloat16)
    rank = jnp.dot(named.astype(jnp.bfloat16), before, preferred_element_type=jnp.float32)
    for k in range(top):
        found = jnp.sum(jnp.where(ids[k : k + 1] == names, rank, 0.0), axis=0, keepdims=True)
        meta_a[z, k : k + 1, :] = ids[k : k + 1] * CAP + found
    meta_a[z, top : 2 * top, :] = weights

    for way, there in enumerate((above, below)):

        @pl.when(there)
        def _():
            meta_copy(way, z).start()

    for way, there, early in ((0, above, low), (1, below, ~low)):

        @pl.when(there & (early | ~above | ~below))
        def _():
            @pl.loop(1, chunks)
            def _(c):
                token_copy(way, z, c).start()


    def own_tokens(c):
        @pl.when(low)
        def _():
            token_copy(1, z, c).start()

        @pl.when(~low)
        def _():
            token_copy(0, z, c).start()

    def pick_table(table, owner):
        want = lax.broadcasted_iota(jnp.int32, (slots, rows), 0).astype(jnp.float32)
        want = want + (owner * slots).astype(jnp.float32)
        hits = [table[k : k + 1] == want for k in range(top)]
        mass = jnp.zeros((slots, rows), jnp.float32)
        for k in range(top):
            mass = jnp.where(hits[k], table[top + k : top + k + 1], mass)
        pick = functools.reduce(jnp.logical_or, hits)
        return jnp.where(pick, 1.0, 0.0).astype(jnp.bfloat16), jnp.sum(mass, axis=1, keepdims=True)

    def put_table(turned, owner):
        want = lax.broadcasted_iota(jnp.int32, (rows, slots), 1).astype(jnp.float32)
        want = want + (owner * slots).astype(jnp.float32)
        pick = functools.reduce(jnp.logical_or, [turned[:, k : k + 1] == want for k in range(top)])
        return jnp.where(pick, 1.0, 0.0).astype(jnp.bfloat16)

    def spread(column):
        return jnp.broadcast_to(column, (slots, 128)).reshape(experts, CAP, 128)

    def take_meta(s):
        @pl.when(s != z)
        def _():
            meta_copy(0, s).wait_recv()

        @pl.when((s < z) & above)
        def _():
            meta_copy(0, s).start()

        @pl.when((s > z) & below)
        def _():
            meta_copy(1, s).start()

        meta_across(s).start()
        table = meta_a[s]
        pick, mass = pick_table(table, ep)
        pick_own[s] = pick
        scale[s, :, :CAP, :] = spread(mass)
        pick_par[s] = pick_table(table, par)[0]
        turned = table.T
        put_own[s] = put_table(turned, ep)
        put_par[s] = put_table(turned, par)

    def take_tokens(s, c):
        @pl.when(s != z)
        def _():
            token_copy(0, s, c).wait_recv()

        @pl.when((s < z) & above)
        def _():
            token_copy(0, s, c).start()

        @pl.when((s > z) & below)
        def _():
            token_copy(1, s, c).start()

        @pl.when(c == 0)
        def _():
            take_meta(s)

        there = jnp.dot(pick_par[s], blk[s, c], preferred_element_type=jnp.float32)
        yout[s, c] = there.astype(jnp.bfloat16)
        give_rows(s, c).start()
        here = jnp.dot(pick_own[s], blk[s, c], preferred_element_type=jnp.float32)
        xa[s, c] = here.astype(jnp.bfloat16)

    tile = min(256, fs)

    def shared_expert():
        for load in loads[:3]:
            load.wait()

        @pl.loop(0, fs // tile)
        def _(k):
            at = pl.ds(pl.multiple_of(k * tile, tile), tile)
            x = jnp.concatenate([blk[z, c] for c in range(chunks)], axis=1)
            g = jnp.dot(x, sg[:, at], preferred_element_type=jnp.float32)
            u = jnp.dot(x, su[:, at], preferred_element_type=jnp.float32)
            hid[:, at] = (jax.nn.silu(g) * u).astype(jnp.bfloat16)

        @pl.loop(0, chunks)
        def _(c):
            at = pl.ds(pl.multiple_of(c * cw, cw), cw)
            shared[c] = jnp.dot(hid[...], sd[:, at], preferred_element_type=jnp.float32)

    def weights_here():
        for load in loads[3:]:
            load.wait()
        for swap in swaps:
            swap.wait_recv()

    gate_sum[...] = jnp.zeros_like(gate_sum)
    up_sum[...] = jnp.zeros_like(up_sum)

    def expert(s, c):
        @pl.when(c == 0)
        def _():
            meta_across(s).wait_recv()
            scale[s, :, CAP:, :] = spread(pick_table(meta_b[s], ep)[1])

        give_rows(s, c).wait_recv()
        depth = pl.ds(pl.multiple_of(c * cw, cw), cw)
        for e in range(experts):
            xcat[e, :CAP, :] = xa[s, c, e * CAP : (e + 1) * CAP, :]
            xcat[e, CAP:, :] = xb[s, c, e * CAP : (e + 1) * CAP, :]
        for e in range(experts):
            for h in range(2):
                gate_sum[h, e] += jnp.dot(xcat[e], wg[h, e, depth, :], preferred_element_type=jnp.float32)
                up_sum[h, e] += jnp.dot(xcat[e], wu[h, e, depth, :], preferred_element_type=jnp.float32)

        @pl.when(c == chunks - 1)
        def _():
            @pl.loop(0, experts)
            def _(e):
                weight = scale[s, e][:, :1]
                for h in range(2):
                    g, u = gate_sum[h, e], up_sum[h, e]
                    hidden[s, h, e] = (jax.nn.silu(g) * u * weight).astype(jnp.bfloat16)
                    gate_sum[h, e] = jnp.zeros_like(g)
                    up_sum[h, e] = jnp.zeros_like(u)

    def give(s, c):
        give_rows(s, c).wait_send()
        at = pl.ds(pl.multiple_of(c * cw, cw), cw)
        for e in range(experts):
            down = jnp.dot(hidden[s, 0, e], wd[0, e, :, at], preferred_element_type=jnp.float32)
            down += jnp.dot(hidden[s, 1, e], wd[1, e, :, at], preferred_element_type=jnp.float32)
            down = down.astype(jnp.bfloat16)
            yout[s, c, e * CAP : (e + 1) * CAP, :] = down[CAP:]
            mine[s, c, e * CAP : (e + 1) * CAP, :] = down[:CAP]
        give_back(s, c).start()

    def total(s, c):
        give_back(s, c).wait_recv()
        own = jnp.dot(put_own[s], mine[s, c], preferred_element_type=jnp.float32)
        own += jnp.dot(put_par[s], back[s, c], preferred_element_type=jnp.float32)
        acc[...] = own

        @pl.when((s >= z) & below)
        def _():
            sum_copy(0, s, c, s).wait_recv()
            acc[...] += rs_in[s, c].astype(jnp.float32)

        @pl.when((s <= z) & above)
        def _():
            slot = jnp.where(s == z, nz, s)
            sum_copy(1, s, c, slot).wait_recv()
            acc[...] += rs_in[slot, c].astype(jnp.float32)

        @pl.when((s < z) & above)
        def _():
            token_copy(0, s, c).wait_send()

        @pl.when((s > z) & below)
        def _():
            token_copy(1, s, c).wait_send()

        @pl.when(s == z)
        def _():
            shared[c] += acc[...]

        @pl.when(s != z)
        def _():
            blk[s, c] = acc[...].astype(jnp.bfloat16)

        @pl.when(s > z)
        def _():
            sum_copy(0, s, c, s).start()

        @pl.when(s < z)
        def _():
            sum_copy(1, s, c, jnp.where(s == z - 1, nz, s)).start()

    def finish():
        @pl.loop(0, rows // step_rows)
        def _(r):
            at = pl.ds(pl.multiple_of(r * step_rows, step_rows), step_rows)
            both = jnp.concatenate([shared[c, at, :] for c in range(chunks)], axis=1)
            out_ref[at, :] = rms_scale(both, pgain_ref[...]).astype(jnp.bfloat16)

    length, step_of = step_tables(nz, chunks, z)

    @pl.loop(0, length)
    def _(k):
        role, s, c = step_of(k)
        pl.when(role == TOKENS_AT)(lambda: take_tokens(s, c))
        pl.when(role == SHARED_AT)(shared_expert)
        pl.when(role == EXPERT_AT)(lambda: expert(s, c))
        pl.when(role == GIVE_AT)(lambda: give(s, c))
        pl.when(role == TOTAL_AT)(lambda: total(s, c))
        pl.when(role == FINISH_AT)(finish)
        pl.when(role == WEIGHTS_AT)(weights_here)
        pl.when(role == OWN_AT)(lambda: own_tokens(c))

    for swap in swaps:
        swap.wait_send()
    for way, there in enumerate((above, below)):

        @pl.when(there)
        def _():
            meta_copy(way, z).wait_send()

            @pl.loop(0, chunks)
            def _(c):
                token_copy(way, z, c).wait_send()

    @pl.loop(0, nz)
    def _(s):
        @pl.when((s < z) & above)
        def _():
            meta_copy(0, s).wait_send()

        @pl.when((s > z) & below)
        def _():
            meta_copy(1, s).wait_send()

        meta_across(s).wait_send()

        @pl.loop(0, chunks)
        def _(c):
            give_back(s, c).wait_send()

            @pl.when(s != z)
            def _():
                sum_copy(0, s, c, s).wait_send()


def grid_shapes(nz, chunks, rows, width, meta_rows, eg, ed, sg, sd):
    bf, f32 = jnp.bfloat16, jnp.float32
    experts = eg.shape[0]
    fs = sg.shape[1]
    cw = width // chunks
    slots = experts * CAP
    return [
        ((2,) + eg.shape, bf),
        ((2,) + eg.shape, bf),
        ((2,) + ed.shape, bf),
        (sg.shape, bf),
        (sg.shape, bf),
        (sd.shape, bf),
        ((nz, chunks, rows, cw), bf),
        ((nz, chunks, slots, cw), bf),
        ((nz, chunks, slots, cw), bf),
        ((experts, 2 * CAP, cw), bf),
        ((2, experts, 2 * CAP, eg.shape[2]), f32),
        ((2, experts, 2 * CAP, eg.shape[2]), f32),
        ((nz, chunks, slots, cw), bf),
        ((nz, chunks, slots, cw), bf),
        ((nz, chunks, slots, cw), bf),
        ((nz, slots, rows), bf),
        ((nz, slots, rows), bf),
        ((nz, rows, slots), bf),
        ((nz, rows, slots), bf),
        ((nz, experts, 2 * CAP, 128), f32),
        ((nz, meta_rows, rows), f32),
        ((nz, meta_rows, rows), f32),
        ((nz + 1, chunks, rows, cw), bf),
        ((chunks, rows, cw), f32),
        ((rows, fs), bf),
        ((nz, 2, experts, 2 * CAP, eg.shape[2]), bf),
        ((rows, cw), f32),
    ]


def grid_body(
    n,
    tokens,
    norm_gain,
    expert_ids,
    gate_weights,
    expert_gate,
    expert_up,
    expert_down,
    shared_gate,
    shared_up,
    shared_down,
    post_gain,
):
    rows, width = tokens.shape
    top = expert_ids.shape[1]
    nz = n // 2
    chunks = CHUNKS
    meta_rows = -(-2 * top // 8) * 8
    shapes = grid_shapes(nz, chunks, rows, width, meta_rows, expert_gate, expert_down, shared_gate, shared_down)
    if ring_bytes(shapes) + 4 * rows * width > VMEM_ALL - (2 << 20):
        return body(
            tokens,
            norm_gain,
            expert_ids,
            gate_weights,
            expert_gate,
            expert_up,
            expert_down,
            shared_gate,
            shared_up,
            shared_down,
            post_gain,
        )
    dma = pltpu.SemaphoreType.DMA
    vmem = pl.BlockSpec(memory_space=pltpu.VMEM)
    hbm = pl.BlockSpec(memory_space=pl.ANY)
    return pl.pallas_call(
        functools.partial(grid_kernel, nz, top, chunks),
        out_shape=jax.ShapeDtypeStruct((rows, width), jnp.bfloat16),
        in_specs=[vmem] * 5 + [hbm] * 6,
        out_specs=vmem,
        scratch_shapes=[pltpu.VMEM(shape, kind) for shape, kind in shapes]
        + [
            dma((6,)),
            dma((3,)),
            dma((3,)),
            dma((2, nz, chunks)),
            dma((nz, chunks)),
            dma((2, nz)),
            dma((nz,)),
            dma((nz,)),
            dma((nz,)),
            dma((nz, chunks)),
            dma((nz, chunks)),
            dma((nz, chunks)),
            dma((nz, chunks)),
            dma((nz, chunks)),
            dma((nz + 1, chunks)),
        ],
        compiler_params=pltpu.CompilerParams(
            collective_id=0, has_side_effects=True, vmem_limit_bytes=VMEM_ALL
        ),
    )(
        tokens,
        expert_ids.T,
        gate_weights.T,
        norm_gain.reshape(1, width),
        post_gain.reshape(1, width),
        expert_gate,
        expert_up,
        expert_down,
        shared_gate,
        shared_up,
        shared_down,
    )


CHUNKS = 4
STEPS = (
    (
        0, 3, 2, 1, 10, 100, 20, 21, 600, 22, 220, 221, 23, 222, 30, 223,
        323, 320, 321, 200, 201, 31, 423, 33, 420, 421, 32, 202, 203, 322, 12, 230,
        231, 232, 233, 333, 422, 331, 332, 11, 433, 210, 431, 13, 330, 211, 432, 212,
        213, 311, 430, 312, 310, 411, 313, 303, 412, 301, 413, 302, 410, 300, 402, 403,
        401, 400, 500,
    ),
    (
        10, 710, 12, 11, 20, 0, 21, 13, 22, 23, 110, 1, 30, 610, 3, 31,
        220, 33, 221, 2, 222, 32, 223, 200, 201, 712, 323, 320, 202, 203, 711, 321,
        230, 713, 423, 231, 232, 322, 420, 233, 210, 211, 330, 333, 332, 421, 331, 212,
        213, 422, 303, 302, 301, 311, 300, 433, 431, 312, 403, 310, 432, 313, 430, 401,
        402, 411, 412, 400, 413, 410, 510,
    ),
)


def ORDERS(nz, chunks, z):
    if nz != 2 * len(STEPS):
        return plain_order(nz, chunks, z)
    near = min(z, nz - 1 - z)
    steps = [(k // 100, k // 10 % 10, k % 10) for k in STEPS[near]]
    return [(role, s if near == z else nz - 1 - s, c) for role, s, c in steps]


def solution(mesh):
    ringed = mesh.shape["tp"] == 2 and mesh.shape["ep"] % 2 == 0 and mesh.shape["ep"] > 2
    return jax.shard_map(
        functools.partial(grid_body, mesh.shape["ep"]) if ringed else body,
        mesh=mesh,
        in_specs=(
            P(("grp", "ep", "tp"), None),
            P(),
            P(("grp", "ep", "tp"), None),
            P(("grp", "ep", "tp"), None),
            P("ep", None, "tp"),
            P("ep", None, "tp"),
            P("ep", "tp", None),
            P(),
            P(),
            P(),
            P(),
        ),
        out_specs=P(("grp", "ep", "tp"), None),
        check_vma=False,
    )
```

```python
import functools

import jax
import jax.numpy as jnp
from jax import lax
from jax.experimental import pallas as pl
from jax.experimental.pallas import tpu as pltpu
from jax.sharding import PartitionSpec as P

EXPERTS = 32
CAP = 40


EPS = 1e-06


def rms_scale(inputs, gain):
    mean_sq = jnp.mean(inputs * inputs, axis=-1, keepdims=True)
    return inputs * lax.rsqrt(mean_sq + EPS) * gain


def expert_rows(tok_rows, w_gate, w_up, w_down):
    gate_act = jnp.einsum("erd,edf->erf", tok_rows, w_gate, preferred_element_type=jnp.float32)
    up_act = jnp.einsum("erd,edf->erf", tok_rows, w_up, preferred_element_type=jnp.float32)
    hidden = (jax.nn.silu(gate_act) * up_act).astype(jnp.bfloat16)
    return jnp.einsum("erf,efd->erd", hidden, w_down, preferred_element_type=jnp.float32)


def shared_branch(normed, shared_gate, shared_up, shared_down):
    shared_act = jnp.dot(normed, shared_gate, preferred_element_type=jnp.float32)
    shared_lift = jnp.dot(normed, shared_up, preferred_element_type=jnp.float32)
    shared_hidden = (jax.nn.silu(shared_act) * shared_lift).astype(jnp.bfloat16)
    return jnp.dot(shared_hidden, shared_down, preferred_element_type=jnp.float32)


def body(
    tokens,
    norm_gain,
    expert_ids,
    gate_weights,
    expert_gate,
    expert_up,
    expert_down,
    shared_gate,
    shared_up,
    shared_down,
    post_gain,
):
    tok_count = tokens.shape[0]
    top_count = expert_ids.shape[1]
    width = tokens.shape[1]
    normed = rms_scale(tokens.astype(jnp.float32), norm_gain).astype(jnp.bfloat16)
    flat_ids = expert_ids.reshape(-1)
    onehot = (flat_ids[:, None] == jnp.arange(EXPERTS, dtype=jnp.int32)[None, :]).astype(jnp.int32)
    slot_index = jnp.sum(jnp.cumsum(onehot, axis=0) * onehot, axis=1) - 1
    position = flat_ids * CAP + slot_index
    source_row = jnp.arange(tok_count * top_count, dtype=jnp.int32) // top_count
    lookup = jnp.full((EXPERTS * CAP,), tok_count, jnp.int32).at[position].set(source_row)
    padded = jnp.concatenate([normed, jnp.zeros((1, width), jnp.bfloat16)], axis=0)
    outgoing = padded[lookup].reshape(EXPERTS, 1, CAP, width)
    whole_gate, whole_up, whole_down = (
        lax.all_gather(expert_gate, "tp", axis=2, tiled=True),
        lax.all_gather(expert_up, "tp", axis=2, tiled=True),
        lax.all_gather(expert_down, "tp", axis=1, tiled=True),
    )
    arrived = lax.all_to_all(outgoing, "ep", split_axis=0, concat_axis=1, tiled=True)
    local_experts = arrived.shape[0]
    senders = arrived.shape[1]
    slots = arrived.shape[2]
    tok_rows = arrived.reshape(local_experts, senders * slots, width)
    result = expert_rows(tok_rows, whole_gate, whole_up, whole_down).astype(jnp.bfloat16)
    result = result.reshape(local_experts, senders, slots, width)
    returned = lax.all_to_all(result, "ep", split_axis=1, concat_axis=0, tiled=True)
    shared_out = shared_branch(normed, shared_gate, shared_up, shared_down)
    back_rows = returned.reshape(EXPERTS * CAP, width)
    picked = back_rows[position].reshape(tok_count, top_count, width).astype(jnp.float32)
    routed = jnp.einsum("tk,tkd->td", gate_weights, picked)
    combined = routed + shared_out
    return rms_scale(combined, post_gain).astype(jnp.bfloat16)

VMEM_ALL = 67043328
MESH = pl.DeviceIdType.MESH


def ring_bytes(shapes):
    total = 0
    for shape, kind in shapes:
        count = jnp.dtype(kind).itemsize
        for size in shape:
            count *= size
        total += count
    return total


ROLES = ("tokens", "shared", "expert", "give", "total", "finish", "weights", "own")
TOKENS_AT, SHARED_AT, EXPERT_AT, GIVE_AT, TOTAL_AT, FINISH_AT, WEIGHTS_AT, OWN_AT = range(8)


def plain_order(nz, chunks, z):
    near = sorted(range(nz), key=lambda s: (abs(s - z), s))
    far = sorted((s for s in range(nz) if s != z), key=lambda s: (-abs(s - z), s)) + [z]
    steps = [(OWN_AT, z, c) for c in range(chunks)] if 0 < z < nz - 1 else []
    steps += [(TOKENS_AT, z, c) for c in range(chunks)] + [(SHARED_AT, z, 0)]
    steps += [(TOKENS_AT, s, c) for s in near[1:2] for c in range(chunks)] + [(WEIGHTS_AT, z, 0)]
    for k, s in enumerate(near):
        steps += [(EXPERT_AT, s, c) for c in range(chunks)]
        if s != z:
            steps += [(GIVE_AT, s, c) for c in range(chunks)]
        steps += [(TOKENS_AT, q, c) for q in near[k + 2 : k + 3] for c in range(chunks)]
    steps += [(GIVE_AT, z, c) for c in range(chunks)]
    steps += [(TOTAL_AT, s, c) for s in far for c in range(chunks)]
    return steps + [(FINISH_AT, z, 0)]


def step_tables(nz, chunks, z):
    orders = [ORDERS(nz, chunks, q) for q in range(nz)]
    length = max(len(order) for order in orders)
    size = len(ROLES) * nz * chunks + 1
    per = 1
    while size ** (per + 1) < 1 << 31:
        per += 1
    count = -(-length // per)
    packed = []
    for order in orders:
        flat = [(role * nz + s) * chunks + c for role, s, c in order]
        flat += [size - 1] * (count * per - len(flat))
        packed.append([sum(v * size**i for i, v in enumerate(flat[k * per : (k + 1) * per])) for k in range(count)])

    def step_of(k):
        group, inside = k // per, k % per
        row = []
        for i in range(count):
            value = jnp.int32(packed[0][i])
            for q in range(1, nz):
                value = jnp.where(z == q, packed[q][i], value)
            row.append(value)
        bit = 1
        while len(row) > 1:
            odd = group // bit % 2 == 1
            row = [jnp.where(odd, row[i + 1], row[i]) if i + 1 < len(row) else row[i] for i in range(0, len(row), 2)]
            bit *= 2
        code = row[0]
        for i in range(per - 1):
            code = jnp.where(inside > i, code // size, code)
        code = code % size
        return code // (nz * chunks), code // chunks % nz, code % chunks

    return length, step_of


def grid_kernel(
    nz,
    top,
    chunks,
    tok_ref,
    ids_ref,
    weights_ref,
    ngain_ref,
    pgain_ref,
    eg_hbm,
    eu_hbm,
    ed_hbm,
    sg_hbm,
    su_hbm,
    sd_hbm,
    out_ref,
    wg,
    wu,
    wd,
    sg,
    su,
    sd,
    blk,
    xa,
    xb,
    xcat,
    gate_sum,
    up_sum,
    yout,
    back,
    mine,
    pick_own,
    pick_par,
    put_own,
    put_par,
    scale,
    meta_a,
    meta_b,
    rs_in,
    shared,
    hid,
    hidden,
    acc,
    load_sem,
    w_send,
    w_recv,
    ag_send,
    ag_recv,
    mt_send,
    mt_recv,
    mb_send,
    mb_recv,
    d_send,
    d_recv,
    r_send,
    r_recv,
    rs_send,
    rs_recv,
):
    rows, width = tok_ref.shape
    experts = eg_hbm.shape[0]
    fh = eg_hbm.shape[2]
    fs = sg.shape[1]
    cw = width // chunks
    slots = experts * CAP
    step_rows = 32
    ep = lax.axis_index("ep")
    tp = lax.axis_index("tp")
    z, y = ep // 2, ep % 2
    par = ep + 1 - 2 * y
    above, below = z < nz - 1, z > 0
    up, dn = jnp.minimum(ep + 2, 2 * nz - 1), jnp.maximum(ep - 2, 0)
    partner = 1 - tp

    barrier = pltpu.get_barrier_semaphore()
    pl.semaphore_signal(barrier, inc=1, device_id={"ep": par}, device_id_type=MESH)
    pl.semaphore_signal(barrier, inc=1, device_id={"tp": partner}, device_id_type=MESH)

    @pl.when(above)
    def _():
        pl.semaphore_signal(barrier, inc=1, device_id={"ep": up}, device_id_type=MESH)

    @pl.when(below)
    def _():
        pl.semaphore_signal(barrier, inc=1, device_id={"ep": dn}, device_id_type=MESH)

    loads = [
        pltpu.make_async_copy(src, dst, load_sem.at[k])
        for k, (src, dst) in enumerate(
            (
                (sg_hbm, sg),
                (su_hbm, su),
                (sd_hbm, sd),
                (eg_hbm, wg.at[0]),
                (eu_hbm, wu.at[0]),
                (ed_hbm, wd.at[0]),
            )
        )
    ]
    for load in loads:
        load.start()

    @pl.loop(0, rows // step_rows)
    def _(r):
        at = pl.ds(pl.multiple_of(r * step_rows, step_rows), step_rows)
        v = rms_scale(tok_ref[at, :].astype(jnp.float32), ngain_ref[...]).astype(jnp.bfloat16)
        for c in range(chunks):
            blk[z, c, at, :] = v[:, c * cw : (c + 1) * cw]

    def remote(src, dst, send, recv, ep_to):
        return pltpu.make_async_remote_copy(
            src_ref=src,
            dst_ref=dst,
            send_sem=send,
            recv_sem=recv,
            device_id={"ep": ep_to},
            device_id_type=MESH,
        )

    def token_copy(way, s, c):
        return remote(blk.at[s, c], blk.at[s, c], ag_send.at[way, s, c], ag_recv.at[s, c], (up, dn)[way])

    def meta_copy(way, s):
        return remote(meta_a.at[s], meta_a.at[s], mt_send.at[way, s], mt_recv.at[s], (up, dn)[way])

    def meta_across(s):
        return remote(meta_a.at[s], meta_b.at[s], mb_send.at[s], mb_recv.at[s], par)

    def give_rows(s, c):
        return remote(yout.at[s, c], xb.at[s, c], d_send.at[s, c], d_recv.at[s, c], par)

    def give_back(s, c):
        return remote(yout.at[s, c], back.at[s, c], r_send.at[s, c], r_recv.at[s, c], par)

    def sum_copy(way, s, c, slot):
        return remote(blk.at[s, c], rs_in.at[slot, c], rs_send.at[s, c], rs_recv.at[slot, c], (up, dn)[way])

    pl.semaphore_wait(barrier, 2 + above.astype(jnp.int32) + below.astype(jnp.int32))

    swaps = [
        pltpu.make_async_remote_copy(
            src_ref=src,
            dst_ref=dst.at[1],
            send_sem=w_send.at[k],
            recv_sem=w_recv.at[k],
            device_id={"tp": partner},
            device_id_type=MESH,
        )
        for k, (src, dst) in enumerate(((eg_hbm, wg), (eu_hbm, wu), (ed_hbm, wd)))
    ]
    for swap in swaps:
        swap.start()

    low = 2 * z < nz
    for way, there, early in ((0, above, low), (1, below, ~low)):

        @pl.when(there & (early | ~above | ~below))
        def _():
            token_copy(way, z, 0).start()

    total_experts = 2 * nz * experts
    ids, weights = ids_ref[...].astype(jnp.float32), weights_ref[...]
    names = lax.broadcasted_iota(jnp.int32, (total_experts, rows), 0).astype(jnp.float32)
    named = jnp.zeros((total_experts, rows), jnp.float32)
    for k in range(top):
        named = jnp.where(ids[k : k + 1] == names, 1.0, named)
    before = lax.broadcasted_iota(jnp.int32, (rows, rows), 0) < lax.broadcasted_iota(jnp.int32, (rows, rows), 1)
    before = jnp.where(before, 1.0, 0.0).astype(jnp.bfloat16)
    rank = jnp.dot(named.astype(jnp.bfloat16), before, preferred_element_type=jnp.float32)
    for k in range(top):
        found = jnp.sum(jnp.where(ids[k : k + 1] == names, rank, 0.0), axis=0, keepdims=True)
        meta_a[z, k : k + 1, :] = ids[k : k + 1] * CAP + found
    meta_a[z, top : 2 * top, :] = weights

    for way, there in enumerate((above, below)):

        @pl.when(there)
        def _():
            meta_copy(way, z).start()

    for way, there, early in ((0, above, low), (1, below, ~low)):

        @pl.when(there & (early | ~above | ~below))
        def _():
            @pl.loop(1, chunks)
            def _(c):
                token_copy(way, z, c).start()


    def own_tokens(c):
        @pl.when(low)
        def _():
            token_copy(1, z, c).start()

        @pl.when(~low)
        def _():
            token_copy(0, z, c).start()

    def pick_table(table, owner):
        want = lax.broadcasted_iota(jnp.int32, (slots, rows), 0).astype(jnp.float32)
        want = want + (owner * slots).astype(jnp.float32)
        hits = [table[k : k + 1] == want for k in range(top)]
        mass = jnp.zeros((slots, rows), jnp.float32)
        for k in range(top):
            mass = jnp.where(hits[k], table[top + k : top + k + 1], mass)
        pick = functools.reduce(jnp.logical_or, hits)
        return jnp.where(pick, 1.0, 0.0).astype(jnp.bfloat16), jnp.sum(mass, axis=1, keepdims=True)

    def put_table(turned, owner):
        want = lax.broadcasted_iota(jnp.int32, (rows, slots), 1).astype(jnp.float32)
        want = want + (owner * slots).astype(jnp.float32)
        pick = functools.reduce(jnp.logical_or, [turned[:, k : k + 1] == want for k in range(top)])
        return jnp.where(pick, 1.0, 0.0).astype(jnp.bfloat16)

    def spread(column):
        return jnp.broadcast_to(column, (slots, 128)).reshape(experts, CAP, 128)

    def take_meta(s):
        @pl.when(s != z)
        def _():
            meta_copy(0, s).wait_recv()

        @pl.when((s < z) & above)
        def _():
            meta_copy(0, s).start()

        @pl.when((s > z) & below)
        def _():
            meta_copy(1, s).start()

        meta_across(s).start()
        table = meta_a[s]
        pick, mass = pick_table(table, ep)
        pick_own[s] = pick
        scale[s, :, :CAP, :] = spread(mass)
        pick_par[s] = pick_table(table, par)[0]
        turned = table.T
        put_own[s] = put_table(turned, ep)
        put_par[s] = put_table(turned, par)

    def take_tokens(s, c):
        @pl.when(s != z)
        def _():
            token_copy(0, s, c).wait_recv()

        @pl.when((s < z) & above)
        def _():
            token_copy(0, s, c).start()

        @pl.when((s > z) & below)
        def _():
            token_copy(1, s, c).start()

        @pl.when(c == 0)
        def _():
            take_meta(s)

        there = jnp.dot(pick_par[s], blk[s, c], preferred_element_type=jnp.float32)
        yout[s, c] = there.astype(jnp.bfloat16)
        give_rows(s, c).start()
        here = jnp.dot(pick_own[s], blk[s, c], preferred_element_type=jnp.float32)
        xa[s, c] = here.astype(jnp.bfloat16)

    tile = min(256, fs)

    def shared_expert():
        for load in loads[:3]:
            load.wait()

        @pl.loop(0, fs // tile)
        def _(k):
            at = pl.ds(pl.multiple_of(k * tile, tile), tile)
            x = jnp.concatenate([blk[z, c] for c in range(chunks)], axis=1)
            g = jnp.dot(x, sg[:, at], preferred_element_type=jnp.float32)
            u = jnp.dot(x, su[:, at], preferred_element_type=jnp.float32)
            hid[:, at] = (jax.nn.silu(g) * u).astype(jnp.bfloat16)

        @pl.loop(0, chunks)
        def _(c):
            at = pl.ds(pl.multiple_of(c * cw, cw), cw)
            shared[c] = jnp.dot(hid[...], sd[:, at], preferred_element_type=jnp.float32)

    def weights_here():
        for load in loads[3:]:
            load.wait()
        for swap in swaps:
            swap.wait_recv()

    gate_sum[...] = jnp.zeros_like(gate_sum)
    up_sum[...] = jnp.zeros_like(up_sum)

    def expert(s, c):
        @pl.when(c == 0)
        def _():
            meta_across(s).wait_recv()
            scale[s, :, CAP:, :] = spread(pick_table(meta_b[s], ep)[1])

        give_rows(s, c).wait_recv()
        depth = pl.ds(pl.multiple_of(c * cw, cw), cw)
        for e in range(experts):
            xcat[e, :CAP, :] = xa[s, c, e * CAP : (e + 1) * CAP, :]
            xcat[e, CAP:, :] = xb[s, c, e * CAP : (e + 1) * CAP, :]
        for e in range(experts):
            for h in range(2):
                gate_sum[h, e] += jnp.dot(xcat[e], wg[h, e, depth, :], preferred_element_type=jnp.float32)
                up_sum[h, e] += jnp.dot(xcat[e], wu[h, e, depth, :], preferred_element_type=jnp.float32)

        @pl.when(c == chunks - 1)
        def _():
            @pl.loop(0, experts)
            def _(e):
                weight = scale[s, e][:, :1]
                for h in range(2):
                    g, u = gate_sum[h, e], up_sum[h, e]
                    hidden[s, h, e] = (jax.nn.silu(g) * u * weight).astype(jnp.bfloat16)
                    gate_sum[h, e] = jnp.zeros_like(g)
                    up_sum[h, e] = jnp.zeros_like(u)

    def give(s, c):
        give_rows(s, c).wait_send()
        at = pl.ds(pl.multiple_of(c * cw, cw), cw)
        for e in range(experts):
            down = jnp.dot(hidden[s, 0, e], wd[0, e, :, at], preferred_element_type=jnp.float32)
            down += jnp.dot(hidden[s, 1, e], wd[1, e, :, at], preferred_element_type=jnp.float32)
            down = down.astype(jnp.bfloat16)
            yout[s, c, e * CAP : (e + 1) * CAP, :] = down[CAP:]
            mine[s, c, e * CAP : (e + 1) * CAP, :] = down[:CAP]
        give_back(s, c).start()

    def total(s, c):
        acc[...] = jnp.dot(put_own[s], mine[s, c], preferred_element_type=jnp.float32)
        give_back(s, c).wait_recv()
        acc[...] += jnp.dot(put_par[s], back[s, c], preferred_element_type=jnp.float32)

        @pl.when((s >= z) & below)
        def _():
            sum_copy(0, s, c, s).wait_recv()
            acc[...] += rs_in[s, c].astype(jnp.float32)

        @pl.when((s <= z) & above)
        def _():
            slot = jnp.where(s == z, nz, s)
            sum_copy(1, s, c, slot).wait_recv()
            acc[...] += rs_in[slot, c].astype(jnp.float32)

        @pl.when((s < z) & above)
        def _():
            token_copy(0, s, c).wait_send()

        @pl.when((s > z) & below)
        def _():
            token_copy(1, s, c).wait_send()

        @pl.when(s == z)
        def _():
            shared[c] += acc[...]

        @pl.when(s != z)
        def _():
            blk[s, c] = acc[...].astype(jnp.bfloat16)

        @pl.when(s > z)
        def _():
            sum_copy(0, s, c, s).start()

        @pl.when(s < z)
        def _():
            sum_copy(1, s, c, jnp.where(s == z - 1, nz, s)).start()

    def finish():
        @pl.loop(0, rows // step_rows)
        def _(r):
            at = pl.ds(pl.multiple_of(r * step_rows, step_rows), step_rows)
            both = jnp.concatenate([shared[c, at, :] for c in range(chunks)], axis=1)
            out_ref[at, :] = rms_scale(both, pgain_ref[...]).astype(jnp.bfloat16)

    length, step_of = step_tables(nz, chunks, z)

    @pl.loop(0, length)
    def _(k):
        role, s, c = step_of(k)
        pl.when(role == TOKENS_AT)(lambda: take_tokens(s, c))
        pl.when(role == SHARED_AT)(shared_expert)
        pl.when(role == EXPERT_AT)(lambda: expert(s, c))
        pl.when(role == GIVE_AT)(lambda: give(s, c))
        pl.when(role == TOTAL_AT)(lambda: total(s, c))
        pl.when(role == FINISH_AT)(finish)
        pl.when(role == WEIGHTS_AT)(weights_here)
        pl.when(role == OWN_AT)(lambda: own_tokens(c))

    for swap in swaps:
        swap.wait_send()
    for way, there in enumerate((above, below)):

        @pl.when(there)
        def _():
            meta_copy(way, z).wait_send()

            @pl.loop(0, chunks)
            def _(c):
                token_copy(way, z, c).wait_send()

    @pl.loop(0, nz)
    def _(s):
        @pl.when((s < z) & above)
        def _():
            meta_copy(0, s).wait_send()

        @pl.when((s > z) & below)
        def _():
            meta_copy(1, s).wait_send()

        meta_across(s).wait_send()

        @pl.loop(0, chunks)
        def _(c):
            give_back(s, c).wait_send()

            @pl.when(s != z)
            def _():
                sum_copy(0, s, c, s).wait_send()


def grid_shapes(nz, chunks, rows, width, meta_rows, eg, ed, sg, sd):
    bf, f32 = jnp.bfloat16, jnp.float32
    experts = eg.shape[0]
    fs = sg.shape[1]
    cw = width // chunks
    slots = experts * CAP
    return [
        ((2,) + eg.shape, bf),
        ((2,) + eg.shape, bf),
        ((2,) + ed.shape, bf),
        (sg.shape, bf),
        (sg.shape, bf),
        (sd.shape, bf),
        ((nz, chunks, rows, cw), bf),
        ((nz, chunks, slots, cw), bf),
        ((nz, chunks, slots, cw), bf),
        ((experts, 2 * CAP, cw), bf),
        ((2, experts, 2 * CAP, eg.shape[2]), f32),
        ((2, experts, 2 * CAP, eg.shape[2]), f32),
        ((nz, chunks, slots, cw), bf),
        ((nz, chunks, slots, cw), bf),
        ((nz, chunks, slots, cw), bf),
        ((nz, slots, rows), bf),
        ((nz, slots, rows), bf),
        ((nz, rows, slots), bf),
        ((nz, rows, slots), bf),
        ((nz, experts, 2 * CAP, 128), f32),
        ((nz, meta_rows, rows), f32),
        ((nz, meta_rows, rows), f32),
        ((nz + 1, chunks, rows, cw), bf),
        ((chunks, rows, cw), f32),
        ((rows, fs), bf),
        ((nz, 2, experts, 2 * CAP, eg.shape[2]), bf),
        ((rows, cw), f32),
    ]


def grid_body(
    n,
    tokens,
    norm_gain,
    expert_ids,
    gate_weights,
    expert_gate,
    expert_up,
    expert_down,
    shared_gate,
    shared_up,
    shared_down,
    post_gain,
):
    rows, width = tokens.shape
    top = expert_ids.shape[1]
    nz = n // 2
    chunks = CHUNKS
    meta_rows = -(-2 * top // 8) * 8
    shapes = grid_shapes(nz, chunks, rows, width, meta_rows, expert_gate, expert_down, shared_gate, shared_down)
    if ring_bytes(shapes) + 4 * rows * width > VMEM_ALL - (2 << 20):
        return body(
            tokens,
            norm_gain,
            expert_ids,
            gate_weights,
            expert_gate,
            expert_up,
            expert_down,
            shared_gate,
            shared_up,
            shared_down,
            post_gain,
        )
    dma = pltpu.SemaphoreType.DMA
    vmem = pl.BlockSpec(memory_space=pltpu.VMEM)
    hbm = pl.BlockSpec(memory_space=pl.ANY)
    return pl.pallas_call(
        functools.partial(grid_kernel, nz, top, chunks),
        out_shape=jax.ShapeDtypeStruct((rows, width), jnp.bfloat16),
        in_specs=[vmem] * 5 + [hbm] * 6,
        out_specs=vmem,
        scratch_shapes=[pltpu.VMEM(shape, kind) for shape, kind in shapes]
        + [
            dma((6,)),
            dma((3,)),
            dma((3,)),
            dma((2, nz, chunks)),
            dma((nz, chunks)),
            dma((2, nz)),
            dma((nz,)),
            dma((nz,)),
            dma((nz,)),
            dma((nz, chunks)),
            dma((nz, chunks)),
            dma((nz, chunks)),
            dma((nz, chunks)),
            dma((nz, chunks)),
            dma((nz + 1, chunks)),
        ],
        compiler_params=pltpu.CompilerParams(
            collective_id=0, has_side_effects=True, vmem_limit_bytes=VMEM_ALL
        ),
    )(
        tokens,
        expert_ids.T,
        gate_weights.T,
        norm_gain.reshape(1, width),
        post_gain.reshape(1, width),
        expert_gate,
        expert_up,
        expert_down,
        shared_gate,
        shared_up,
        shared_down,
    )


CHUNKS = 4
STEPS = (
    (
        0, 3, 2, 1, 10, 100, 20, 21, 600, 22, 220, 221, 23, 222, 30, 223,
        323, 320, 321, 200, 201, 31, 423, 33, 420, 421, 32, 202, 203, 322, 12, 230,
        231, 232, 233, 333, 422, 331, 332, 11, 433, 210, 431, 13, 330, 211, 432, 212,
        213, 311, 430, 312, 310, 411, 313, 303, 412, 301, 413, 302, 410, 300, 402, 403,
        401, 400, 500,
    ),
    (
        10, 710, 12, 11, 20, 0, 21, 13, 22, 23, 110, 1, 30, 610, 3, 31,
        220, 33, 221, 2, 222, 32, 223, 200, 201, 712, 323, 320, 202, 203, 711, 321,
        230, 713, 423, 231, 232, 322, 420, 233, 210, 211, 330, 333, 332, 421, 331, 212,
        213, 422, 303, 302, 301, 311, 300, 433, 431, 312, 403, 310, 432, 313, 430, 401,
        402, 411, 412, 400, 413, 410, 510,
    ),
)


def ORDERS(nz, chunks, z):
    if nz != 2 * len(STEPS):
        return plain_order(nz, chunks, z)
    near = min(z, nz - 1 - z)
    steps = [(k // 100, k // 10 % 10, k % 10) for k in STEPS[near]]
    return [(role, s if near == z else nz - 1 - s, c) for role, s, c in steps]


def solution(mesh):
    ringed = mesh.shape["tp"] == 2 and mesh.shape["ep"] % 2 == 0 and mesh.shape["ep"] > 2
    return jax.shard_map(
        functools.partial(grid_body, mesh.shape["ep"]) if ringed else body,
        mesh=mesh,
        in_specs=(
            P(("grp", "ep", "tp"), None),
            P(),
            P(("grp", "ep", "tp"), None),
            P(("grp", "ep", "tp"), None),
            P("ep", None, "tp"),
            P("ep", None, "tp"),
            P("ep", "tp", None),
            P(),
            P(),
            P(),
            P(),
        ),
        out_specs=P(("grp", "ep", "tp"), None),
        check_vma=False,
    )
```
